32 devices in a mesh: fs: 8 (over z, y), tp: 4 (over x, core).
Axes of the slice: x: 2, y: 2, z: 4, core: 2. Of those that a mesh axis runs over, the one named last changes fastest.
Arguments:
- tokens: bfloat16 [3072, 2048], P('fs'), may hold values from -6 to 6
- first_norm_scale: float32 [2048], replicated, may hold values from 0.1 to 1.9
- recurrent_branch_matrix: bfloat16 [2048, 1024], P('fs', 'tp'), may hold values from -0.125 to 0.125
- gelu_gate_matrix: bfloat16 [2048, 1024], P('fs', 'tp'), may hold values from -0.125 to 0.125
- filter_taps_weight: bfloat16 [4, 1024], P(None, 'tp'), may hold values from -3 to 3
- recurrence_gate_blocks: bfloat16 [16, 64, 64], P('tp'), may hold values from -0.75 to 0.75
- input_gate_blocks: bfloat16 [16, 64, 64], P('tp'), may hold values from -0.75 to 0.75
- base_decay_logits: float32 [1024], P('tp'), may hold values from 4 to 11
- extra_log_decay: float32 [3072, 1024], P('fs', 'tp'), may hold values from -0.7 to 0
- mixer_output_matrix: bfloat16 [2048, 1024], P('fs', 'tp'), may hold values from -0.5 to 0.5
- second_norm_scale: float32 [2048], replicated, may hold values from 0.1 to 1.9
- mixer_up_matrix: bfloat16 [2048, 4096], P('fs', 'tp'), may hold values from -0.125 to 0.125
- mixer_down_matrix: bfloat16 [2048, 4096], P('fs', 'tp'), may hold values from -0.09375 to 0.09375
Outputs:
- layer_out: bfloat16 [3072, 2048], P(('fs', 'tp'))
The draws below stay inside these ranges and needn't reach their ends.
All inputs are finite; a program needn't handle non-finite values.
Results may differ from the reference program's by a relative error of at most 0.022.
Values may be sent and summed in bfloat16 or wider, within the bound.
A program may use at most 64 MiB of HBM per device.

```python
import jax
import jax.numpy as jnp
from jax import lax

D = 2048
R_BLOCKS = 16
BLOCK_DIM = 64
RECURRENT_WIDTH = 1024
FF = 4096
TAPS = 4
SEQUENCE_LENGTH = 384
TOKENS = 3072
N_FS = 8
N_TP = 4


def draw_base_decay_logits(key, part):
    pick_key, quick_key, slow_key = jax.random.split(jax.random.fold_in(key, 11), 3)
    quick_share = 0.5
    quick_mask = jax.random.uniform(pick_key, (RECURRENT_WIDTH,), jnp.float32) < quick_share
    quick_speed = jnp.exp(jax.random.uniform(quick_key, (RECURRENT_WIDTH,), jnp.float32, jnp.log(0.004), jnp.log(0.012)))
    slow_speed = jnp.exp(jax.random.uniform(slow_key, (RECURRENT_WIDTH,), jnp.float32, jnp.log(0.03), jnp.log(0.25))) / SEQUENCE_LENGTH
    speeds = jnp.where(quick_mask, quick_speed, slow_speed)
    return (-speeds - jnp.log(-jnp.expm1(-speeds))).astype(jnp.float32)


def draw_extra_log_decay(key, part):
    place_key, depth_key = jax.random.split(jax.random.fold_in(key, 23))
    marked = jax.random.uniform(place_key, (TOKENS, 1), jnp.float32) < 4.0 / SEQUENCE_LENGTH
    kept = jax.random.uniform(depth_key, (TOKENS, RECURRENT_WIDTH), jnp.float32, 0.5, 0.8)
    return jnp.where(marked, jnp.log(kept), 0.0).astype(jnp.float32)


def steps_of(key, shape, shards, smallest, top_value):
    factor_of, own = 1.0, jax.random.fold_in(key, 6)
    for dim, parts in shards:
        steps = jnp.exp(jax.random.uniform(jax.random.fold_in(own, dim), (parts,), jnp.float32, smallest / len(shards), top_value / len(shards)))
        factor_of = factor_of * jnp.repeat(steps, shape[dim] // parts).reshape([-1 if axis == dim else 1 for axis in range(len(shape))])
    return factor_of


def noise(rng, dims, spread, most, shards=(), dtype=jnp.bfloat16):
    values = jax.random.normal(rng, dims, jnp.float32) * spread
    if len(shards) > 0:
        values = steps_of(rng, dims, shards, -0.22, 0.18) * values
    return jnp.clip(values, min=-most, max=most).astype(dtype)


def setup_inputs(seed: int = 0) -> dict:
    keys = jax.random.split(jax.random.key(seed), 14)
    tokens = noise(keys[0], (TOKENS, D), 1.0, 6.0, ((0, 8),))
    first_norm_scale = jnp.clip(1.0 + 0.18 * jax.random.normal(keys[1], (D,), jnp.float32), 0.1, 1.9)
    recurrent_branch_matrix = noise(keys[2], (D, RECURRENT_WIDTH), D ** -0.5, 0.125, ((0, 8), (1, 4)))
    gelu_gate_matrix = noise(keys[3], (D, RECURRENT_WIDTH), D ** -0.5, 0.125, ((0, 8), (1, 4)))
    filter_taps_weight = noise(keys[4], (TAPS, RECURRENT_WIDTH), TAPS ** -0.5, 3.0, ((1, 4),))
    recurrence_gate_blocks = noise(keys[5], (R_BLOCKS, BLOCK_DIM, BLOCK_DIM), BLOCK_DIM ** -0.5, 0.75, ((0, 4),))
    input_gate_blocks = noise(keys[6], (R_BLOCKS, BLOCK_DIM, BLOCK_DIM), BLOCK_DIM ** -0.5, 0.75, ((0, 4),))
    base_decay_logits = draw_base_decay_logits(jax.random.fold_in(keys[13], 71), 0)
    extra_log_decay = draw_extra_log_decay(jax.random.fold_in(keys[13], 71), 0)
    mixer_output_matrix = noise(keys[9], (D, RECURRENT_WIDTH), (RECURRENT_WIDTH // 9) ** -0.5, 0.5, ((0, 8), (1, 4)))
    second_norm_scale = jnp.clip(1.0 + 0.18 * jax.random.normal(keys[10], (D,), jnp.float32), 0.1, 1.9)
    mixer_up_matrix = noise(keys[11], (D, FF), D ** -0.5, 0.125, ((0, 8), (1, 4)))
    mixer_down_matrix = noise(keys[12], (D, FF), FF ** -0.5, 0.09375, ((0, 8), (1, 4)))
    return dict(tokens=tokens, first_norm_scale=first_norm_scale, recurrent_branch_matrix=recurrent_branch_matrix, gelu_gate_matrix=gelu_gate_matrix, filter_taps_weight=filter_taps_weight, recurrence_gate_blocks=recurrence_gate_blocks, input_gate_blocks=input_gate_blocks, base_decay_logits=base_decay_logits, extra_log_decay=extra_log_decay, mixer_output_matrix=mixer_output_matrix, second_norm_scale=second_norm_scale, mixer_up_matrix=mixer_up_matrix, mixer_down_matrix=mixer_down_matrix)


epsilon = 1e-06
decay_rate_scale = 8.0

def rms_scaled(sequence_token_rows, scales):
    widened = sequence_token_rows.astype(jnp.float32)
    mean_square = lax.optimization_barrier(jnp.mean(widened * widened, axis=-1, keepdims=True))
    return (widened * lax.rsqrt(mean_square + epsilon) * scales).astype(jnp.bfloat16)

def linear_combine(earlier, later):
    return (earlier[0] * later[0], later[0] * earlier[1] + later[1])

def causal_taps(branch, filter_taps_weight):
    tap_count = filter_taps_weight.shape[0]
    positions = branch.shape[0]
    padded = jnp.pad(branch.astype(jnp.float32), ((tap_count - 1, 0), (0, 0)))
    running = jnp.zeros(branch.shape, jnp.float32)
    for offset in range(tap_count):
        running = running + padded[offset:offset + positions] * filter_taps_weight[offset].astype(jnp.float32)
    return running.astype(jnp.bfloat16)

def block_map(convolved, blocks):
    positions, channels = convolved.shape
    grouped = convolved.astype(jnp.float32).reshape(positions, blocks.shape[0], blocks.shape[1])
    mapped = jnp.einsum('sgi,gij->sgj', grouped, blocks.astype(jnp.float32))
    return jax.nn.sigmoid(mapped.reshape(positions, channels))

def grouped_sum(left, right, groups):
    width_each = left.shape[1] // groups
    running = jnp.zeros((left.shape[0], right.shape[0]), jnp.float32)
    for column_group in range(groups):
        begin_col = column_group * width_each
        partial_value = jnp.dot(left[:, begin_col:begin_col + width_each], right[:, begin_col:begin_col + width_each].T, preferred_element_type=jnp.float32)
        rounded = lax.optimization_barrier(partial_value.astype(jnp.bfloat16))
        running = running + rounded.astype(jnp.float32)
    return running

def reference(tokens, first_norm_scale, recurrent_branch_matrix, gelu_gate_matrix, filter_taps_weight, recurrence_gate_blocks, input_gate_blocks, base_decay_logits, extra_log_decay, mixer_output_matrix, second_norm_scale, mixer_up_matrix, mixer_down_matrix):

    def single_sequence(input_values):
        sequence_token_rows, extra_decays = input_values
        normed = rms_scaled(sequence_token_rows, first_norm_scale)
        branch = jnp.dot(normed, recurrent_branch_matrix, preferred_element_type=jnp.float32).astype(jnp.bfloat16)
        gate_branch = jnp.dot(normed, gelu_gate_matrix, preferred_element_type=jnp.float32).astype(jnp.bfloat16)
        convolved = causal_taps(branch, filter_taps_weight)
        recurrence_gate_value = block_map(convolved, recurrence_gate_blocks)
        admission = block_map(convolved, input_gate_blocks)
        log_keep_factor = decay_rate_scale * recurrence_gate_value * jax.nn.log_sigmoid(base_decay_logits) + extra_decays
        retain = jnp.exp(log_keep_factor)
        driven = jnp.sqrt(-jnp.expm1(2.0 * log_keep_factor)) * (admission * convolved.astype(jnp.float32))
        memory = lax.associative_scan(linear_combine, (retain, driven), axis=0)[1]
        recurrent = (memory * jax.nn.gelu(gate_branch.astype(jnp.float32))).astype(jnp.bfloat16)
        mixer_out = grouped_sum(recurrent, mixer_output_matrix, N_TP)
        residual = (sequence_token_rows.astype(jnp.float32) + mixer_out).astype(jnp.bfloat16)
        normed_mid = rms_scaled(residual, second_norm_scale)
        raised = jnp.dot(normed_mid, mixer_up_matrix, preferred_element_type=jnp.float32)
        hidden = jnp.square(jax.nn.relu(raised)).astype(jnp.bfloat16)
        channel_sum = grouped_sum(hidden, mixer_down_matrix, N_TP)
        return (residual.astype(jnp.float32) + channel_sum).astype(jnp.bfloat16)
    reshaped_values = tokens.reshape(N_FS, SEQUENCE_LENGTH, D)
    extra_decay_reshaped = extra_log_decay.reshape(N_FS, SEQUENCE_LENGTH, RECURRENT_WIDTH)
    output_values = lax.map(single_sequence, (reshaped_values, extra_decay_reshaped))
    return output_values.reshape(N_FS * SEQUENCE_LENGTH, D)
```

```python
import functools

import jax
import jax.numpy as jnp
from jax import lax
from jax.experimental import pallas as pl
from jax.experimental.pallas import tpu as pltpu
from jax.sharding import PartitionSpec as P

epsilon = 1e-06
decay_rate_scale = 8.0


def rms_scaled(sequence_token_rows, scales):
    widened = sequence_token_rows.astype(jnp.float32)
    mean_square = jnp.mean(widened * widened, axis=-1, keepdims=True)
    return (widened * lax.rsqrt(mean_square + epsilon) * scales).astype(jnp.bfloat16)


def linear_combine(earlier, later):
    return (earlier[0] * later[0], later[0] * earlier[1] + later[1])


def causal_taps(branch, filter_taps_weight):
    tap_count = filter_taps_weight.shape[0]
    positions = branch.shape[0]
    padded = jnp.pad(branch.astype(jnp.float32), ((tap_count - 1, 0), (0, 0)))
    running = jnp.zeros(branch.shape, jnp.float32)
    for offset in range(tap_count):
        running = running + padded[offset : offset + positions] * filter_taps_weight[offset].astype(
            jnp.float32
        )
    return running.astype(jnp.bfloat16)


def block_map(convolved, blocks):
    positions, channels = convolved.shape
    grouped = convolved.reshape(positions, blocks.shape[0], blocks.shape[1])
    mapped = jnp.einsum("sgi,gij->sgj", grouped, blocks, preferred_element_type=jnp.float32)
    return jax.nn.sigmoid(mapped.reshape(positions, channels))


def contract_columns(left, right):
    return lax.dot_general(
        left, right, (((1,), (1,)), ((), ())), preferred_element_type=jnp.float32
    )


def local(
    tokens,
    first_norm_scale,
    recurrent_branch_matrix,
    gelu_gate_matrix,
    filter_taps_weight,
    recurrence_gate_blocks,
    input_gate_blocks,
    base_decay_logits,
    extra_log_decay,
    mixer_output_matrix,
    second_norm_scale,
    mixer_up_matrix,
    mixer_down_matrix,
):
    positions = tokens.shape[0]
    own_count = positions // lax.axis_size("tp")
    normed = rms_scaled(tokens, first_norm_scale)
    branch_sum = jnp.dot(
        normed,
        lax.all_gather(recurrent_branch_matrix, "fs", axis=0, tiled=True),
        preferred_element_type=jnp.float32,
    )
    gate_sum = jnp.dot(
        normed,
        lax.all_gather(gelu_gate_matrix, "fs", axis=0, tiled=True),
        preferred_element_type=jnp.float32,
    )
    branch = branch_sum.astype(jnp.bfloat16)
    gate_branch = gate_sum.astype(jnp.bfloat16)
    out_full = lax.all_gather(mixer_output_matrix, "fs", axis=0, tiled=True)
    convolved = causal_taps(branch, filter_taps_weight)
    recurrence_gate_value = block_map(convolved, recurrence_gate_blocks)
    admission = block_map(convolved, input_gate_blocks)
    log_keep_factor = (
        decay_rate_scale * recurrence_gate_value * jax.nn.log_sigmoid(base_decay_logits)
        + extra_log_decay
    )
    retain = jnp.exp(log_keep_factor)
    driven = jnp.sqrt(-jnp.expm1(2.0 * log_keep_factor)) * (
        admission * convolved.astype(jnp.float32)
    )
    memory = lax.associative_scan(linear_combine, (retain, driven), axis=0)[1]
    recurrent = (memory * jax.nn.gelu(gate_branch.astype(jnp.float32))).astype(jnp.bfloat16)
    up_full = lax.all_gather(mixer_up_matrix, "fs", axis=0, tiled=True)
    whole_sum = lax.psum(contract_columns(recurrent, out_full).astype(jnp.bfloat16), "tp").astype(
        jnp.float32
    )
    residual_all = (tokens.astype(jnp.float32) + whole_sum).astype(jnp.bfloat16)
    raised = jnp.dot(
        rms_scaled(residual_all, second_norm_scale), up_full, preferred_element_type=jnp.float32
    )
    hidden = jnp.square(jax.nn.relu(raised)).astype(jnp.bfloat16)
    residual = lax.dynamic_slice_in_dim(
        residual_all, lax.axis_index("tp") * own_count, own_count, 0
    )
    down_full = lax.all_gather(mixer_down_matrix, "fs", axis=0, tiled=True)
    channel_sum = lax.psum_scatter(
        contract_columns(hidden, down_full).astype(jnp.bfloat16),
        "tp",
        scatter_dimension=0,
        tiled=True,
    ).astype(jnp.float32)
    return (residual.astype(jnp.float32) + channel_sum).astype(jnp.bfloat16)


MESH = pl.DeviceIdType.MESH
Y_SIZE = 2
GROUPS = 4


def fits(mesh):
    n_fs, n_tp = mesh.shape["fs"], mesh.shape["tp"]
    return n_tp == 2 * Y_SIZE and n_fs == 4 * Y_SIZE


def shifted_down(values, by, fill):
    if by % 8 == 0:
        top = jnp.full((by, values.shape[1]), fill, values.dtype)
        return jnp.concatenate([top, values[: values.shape[0] - by]], axis=0)
    rows = lax.broadcasted_iota(jnp.int32, values.shape, 0)
    return jnp.where(rows < by, fill, pltpu.roll(values, by, 0))


def one_minus_exp(exponent):
    series = 1.0
    for order in range(8, 1, -1):
        series = 1.0 + exponent * (1.0 / order) * series
    return jnp.where(exponent > -0.35, -exponent * series, 1.0 - jnp.exp(exponent))


def fused(
    nz,
    tok, scale1, wb, wg, taps, rblk, iblk, logits, extra, wo, scale2, wu, wd,
    out,
    normed, fb, fg, fo, fu, fd, rdiag, idiag,
    part, pair1, give2, got2, res, mid, hidden,
    part_f, pair_f, give_f, got_f,
    send_sem, recv_sem, a_send, a_recv, b_send, b_recv,
):
    f = lax.axis_index("fs")
    t = lax.axis_index("tp")
    z, y = f // Y_SIZE, f % Y_SIZE
    x, c = t // 2, t % 2
    last = nz - 1
    ymate = z * Y_SIZE + (1 - y)
    xmate = (1 - x) * 2 + c
    cmate = x * 2 + (1 - c)
    rows, width = tok.shape
    own_rows = out.shape[0]
    depth = wb.shape[0]
    half = depth // 2

    barrier = pltpu.get_barrier_semaphore()
    zup = lax.rem(z + 1, nz) * Y_SIZE + y
    zdown = lax.rem(z + nz - 1, nz) * Y_SIZE + y
    for other in (zup, zdown, ymate):
        pl.semaphore_signal(barrier, inc=1, device_id={"fs": other, "tp": t}, device_id_type=MESH)
    for other in (xmate, cmate):
        pl.semaphore_signal(barrier, inc=1, device_id={"fs": f, "tp": other}, device_id_type=MESH)
    pl.semaphore_wait(barrier, 5)

    pieces = (
        (wb, fb, 0, depth, False),
        (wg, fg, 0, depth, False),
        (wo, fo, 0, depth, False),
        (wu, fu, 0, half, False),
        (wu, fu, half, half, True),
        (wd, fd, 0, half, False),
        (wd, fd, half, half, True),
    )
    sent = []

    def slot(g, shard):
        _, full, first, count, _ = pieces[g]
        return full.at[pl.ds(pl.multiple_of(shard * depth + first, half), count), :]

    def give(g, shard, way, pred, source=None):
        target = (zup, zdown, ymate)[way]
        here = slot(g, shard)
        copy = pltpu.make_async_remote_copy(
            src_ref=here if source is None else source,
            dst_ref=here,
            send_sem=send_sem.at[g, shard, way],
            recv_sem=recv_sem.at[g, shard],
            device_id={"fs": target, "tp": t},
            device_id_type=MESH,
        )
        if pred is None:
            copy.start()
            sent.append((None, copy))
        else:
            pl.when(pred)(copy.start)
            sent.append((pred, copy))

    def take(g, shard):
        here = slot(g, shard)
        pltpu.make_async_remote_copy(
            src_ref=here,
            dst_ref=here,
            send_sem=send_sem.at[g, shard, 0],
            recv_sem=recv_sem.at[g, shard],
            device_id={"fs": ymate, "tp": t},
            device_id_type=MESH,
        ).wait_recv()

    def own(g):
        w, _, first, count, _ = pieces[g]
        source = w.at[pl.ds(first, count), :]
        give(g, f, 0, z < last, source)
        give(g, f, 1, z > 0, source)
        give(g, f, 2, None, source)

    def wave(g, d):
        along = pieces[g][4]
        for way in (0, 1):
            edge = 0 if way == 0 else last
            zs = z - d if way == 0 else z + d
            exists = zs >= 0 if way == 0 else zs <= last
            onward = z < last if way == 0 else z > 0
            if d > 0:
                shard = zs * Y_SIZE + y
                pl.when(exists)(functools.partial(take, g, shard))
                give(g, shard, way, exists & onward)
                if along:
                    give(g, shard, 2, exists & (zs != 0) & (zs != last))
                else:
                    give(g, shard, 2, exists)
            if along:
                outer = zs == edge
                shard = edge * Y_SIZE + (1 - y)
                pl.when(outer)(functools.partial(take, g, shard))
                give(g, shard, way, outer & onward)

    def take_across(g):
        for zs in range(nz):
            if not (pieces[g][4] and zs in (0, last)):
                take(g, zs * Y_SIZE + (1 - y))

    def tp_copy(source, target, other, index, send, recv):
        return pltpu.make_async_remote_copy(
            src_ref=source,
            dst_ref=target,
            send_sem=send.at[index],
            recv_sem=recv.at[index],
            device_id={"fs": f, "tp": other},
            device_id_type=MESH,
        )

    own(0)
    own(1)
    own(2)
    own(3)

    place = pl.ds(pl.multiple_of(f * depth, depth), depth)
    fb[place, :] = wb[...]
    fg[place, :] = wg[...]
    fo[place, :] = wo[...]
    fu[place, :] = wu[...]
    fd[place, :] = wd[...]
    block = rblk.shape[1]
    for blocks, diag in ((rblk, rdiag), (iblk, idiag)):
        diag[...] = jnp.zeros_like(diag)
        for b in range(rblk.shape[0]):
            diag[b * block : (b + 1) * block, b * block : (b + 1) * block] = blocks[b]

    def norm_rows(i, carry):
        at = pl.ds(pl.multiple_of(i * 32, 32), 32)
        normed[at, :] = rms_scaled(tok[at, :], scale1[...])
        return carry

    lax.fori_loop(0, rows // 32, norm_rows, 0)

    for d in range(1, nz):
        wave(0, d)
        wave(1, d)
    own(4)
    wave(2, 1)
    take_across(0)
    take_across(1)

    branch = jnp.dot(normed[...], fb[...], preferred_element_type=jnp.float32)
    branch = branch.astype(jnp.bfloat16).astype(jnp.float32)
    tap_count = taps.shape[0]
    running = branch * taps[tap_count - 1 : tap_count, :].astype(jnp.float32)
    for offset in range(tap_count - 1):
        by = tap_count - 1 - offset
        running = running + shifted_down(branch, by, 0.0) * taps[offset : offset + 1, :].astype(
            jnp.float32
        )
    convolved = running.astype(jnp.bfloat16)
    rate = jax.nn.sigmoid(jnp.dot(convolved, rdiag[...], preferred_element_type=jnp.float32))
    admission = jax.nn.sigmoid(jnp.dot(convolved, idiag[...], preferred_element_type=jnp.float32))
    base = -jnp.log1p(jnp.exp(-logits[...]))
    log_keep = decay_rate_scale * rate * base + extra[...]
    keep = jnp.exp(log_keep)
    memory = jnp.sqrt(one_minus_exp(2.0 * log_keep)) * (admission * convolved.astype(jnp.float32))
    by = 1
    while by < rows:
        memory = keep * shifted_down(memory, by, 0.0) + memory
        if 2 * by < rows:
            keep = keep * shifted_down(keep, by, 1.0)
        by *= 2
    gate = jnp.dot(normed[...], fg[...], preferred_element_type=jnp.float32)
    gate = gate.astype(jnp.bfloat16).astype(jnp.float32)
    recurrent = (memory * jax.nn.gelu(gate)).astype(jnp.bfloat16)

    wave(2, 2)
    wave(2, 3)
    wave(3, 1)
    own(5)
    take_across(2)
    for k in range(width // depth):
        product = contract_columns(recurrent, fo[k * depth : (k + 1) * depth, :])
        part[:, :, k * depth : (k + 1) * depth] = product.astype(jnp.bfloat16).reshape(
            part.shape[0], own_rows, depth
        )
    first = [
        tp_copy(part.at[2 * other + (1 - c)], pair1.at[other], cmate, other, a_send, a_recv)
        for other in range(2)
    ]
    for copy in first:
        copy.start()
    wave(3, 2)
    for copy in first:
        copy.wait_recv()
    away = part[2 * (1 - x) + c].astype(jnp.float32) + pair1[1 - x].astype(jnp.float32)
    give2[...] = away.astype(jnp.bfloat16)
    second = tp_copy(give2, got2, xmate, 2, a_send, a_recv)
    second.start()
    own(6)
    wave(3, 3)
    wave(4, 0)
    wave(4, 1)
    second.wait_recv()
    own_at = pl.ds(pl.multiple_of(t * own_rows, own_rows), own_rows)
    mixed = part[t].astype(jnp.float32) + pair1[x].astype(jnp.float32)
    mixed = mixed + got2[...].astype(jnp.float32)
    residual = (tok[own_at, :].astype(jnp.float32) + mixed).astype(jnp.bfloat16)
    res[...] = residual
    mid[t] = rms_scaled(residual, scale2[...])
    spread = [
        tp_copy(mid.at[t], mid.at[t], xmate, 3, a_send, a_recv),
        tp_copy(mid.at[t], mid.at[t], cmate, 4, a_send, a_recv),
    ]
    for copy in spread:
        copy.start()
    wave(4, 2)
    wave(5, 1)
    tp_copy(mid.at[xmate], mid.at[xmate], xmate, 3, a_send, a_recv).wait_recv()
    relay = tp_copy(mid.at[xmate], mid.at[xmate], cmate, 5, a_send, a_recv)
    relay.start()
    wave(4, 3)
    wave(5, 2)
    tp_copy(mid.at[cmate], mid.at[cmate], cmate, 4, a_send, a_recv).wait_recv()
    diagonal = (1 - x) * 2 + (1 - c)
    tp_copy(mid.at[diagonal], mid.at[diagonal], cmate, 5, a_send, a_recv).wait_recv()
    take_across(3)
    take_across(4)

    tile = 256

    def up_tile(i, carry):
        at = pl.ds(pl.multiple_of(i * tile, tile), tile)
        raised = jnp.dot(
            mid[...].reshape(rows, width), fu[:, at], preferred_element_type=jnp.float32
        )
        hidden[:, at] = jnp.square(jnp.maximum(raised, 0.0)).astype(jnp.bfloat16)
        return carry

    lax.fori_loop(0, fu.shape[1] // tile, up_tile, 0)

    wave(5, 3)
    for d in range(nz):
        wave(6, d)

    span = width // GROUPS
    side = z // (nz // 2)
    firsts, seconds = [], []

    def finish_first(j):
        for copy in firsts[j]:
            copy.wait_recv()
        away = part_f[j, 2 * (1 - x) + c].astype(jnp.float32) + pair_f[j, 1 - x].astype(jnp.float32)
        give_f[j] = away.astype(jnp.bfloat16)
        copy = tp_copy(give_f.at[j], got_f.at[j], xmate, 3 * j + 2, b_send, b_recv)
        copy.start()
        seconds.append(copy)

    def columns(j):
        return pl.ds(pl.multiple_of((j + side * (last - 2 * j)) * span, span), span)

    def finish_second(j):
        seconds[j].wait_recv()
        total = part_f[j, t].astype(jnp.float32) + pair_f[j, x].astype(jnp.float32)
        total = total + got_f[j].astype(jnp.float32)
        out[:, columns(j)] = (res[:, columns(j)].astype(jnp.float32) + total).astype(jnp.bfloat16)

    for j in range(GROUPS):
        q = j + side * (last - 2 * j)
        take(5, q * Y_SIZE + (1 - y))
        if j not in (0, last):
            take(6, q * Y_SIZE + (1 - y))
        product = contract_columns(hidden[...], fd[columns(j), :])
        part_f[j] = product.astype(jnp.bfloat16).reshape(part.shape[0], own_rows, span)
        copies = [
            tp_copy(
                part_f.at[j, 2 * other + (1 - c)], pair_f.at[j, other], cmate, 3 * j + other,
                b_send, b_recv,
            )
            for other in range(2)
        ]
        for copy in copies:
            copy.start()
        firsts.append(copies)
        if j > 0:
            finish_first(j - 1)
    finish_first(GROUPS - 1)
    for j in range(GROUPS):
        finish_second(j)

    for pred, copy in sent:
        if pred is None:
            copy.wait_send()
        else:
            pl.when(pred)(copy.wait_send)
    for copy in first + [second] + spread + [relay] + seconds:
        copy.wait_send()
    for copies in firsts:
        for copy in copies:
            copy.wait_send()


def fused_local(
    mesh,
    tokens,
    first_norm_scale,
    recurrent_branch_matrix,
    gelu_gate_matrix,
    filter_taps_weight,
    recurrence_gate_blocks,
    input_gate_blocks,
    base_decay_logits,
    extra_log_decay,
    mixer_output_matrix,
    second_norm_scale,
    mixer_up_matrix,
    mixer_down_matrix,
):
    n_fs, n_tp = mesh.shape["fs"], mesh.shape["tp"]
    rows, width = tokens.shape
    own_rows = rows // n_tp
    channels = recurrent_branch_matrix.shape[1]
    units = mixer_up_matrix.shape[1]
    span = width // GROUPS
    low, high = jnp.bfloat16, jnp.float32
    vmem = pl.BlockSpec(memory_space=pltpu.VMEM)
    return pl.pallas_call(
        functools.partial(fused, n_fs // Y_SIZE),
        out_shape=jax.ShapeDtypeStruct((own_rows, width), low),
        in_specs=[vmem] * 13,
        out_specs=vmem,
        scratch_shapes=[
            pltpu.VMEM((rows, width), low),
            pltpu.VMEM((width, channels), low),
            pltpu.VMEM((width, channels), low),
            pltpu.VMEM((width, channels), low),
            pltpu.VMEM((width, units), low),
            pltpu.VMEM((width, units), low),
            pltpu.VMEM((channels, channels), low),
            pltpu.VMEM((channels, channels), low),
            pltpu.VMEM((n_tp, own_rows, width), low),
            pltpu.VMEM((2, own_rows, width), low),
            pltpu.VMEM((own_rows, width), low),
            pltpu.VMEM((own_rows, width), low),
            pltpu.VMEM((own_rows, width), low),
            pltpu.VMEM((n_tp, own_rows, width), low),
            pltpu.VMEM((rows, units), low),
            pltpu.VMEM((GROUPS, n_tp, own_rows, span), low),
            pltpu.VMEM((GROUPS, 2, own_rows, span), low),
            pltpu.VMEM((GROUPS, own_rows, span), low),
            pltpu.VMEM((GROUPS, own_rows, span), low),
            pltpu.SemaphoreType.DMA((7, n_fs, 3)),
            pltpu.SemaphoreType.DMA((7, n_fs)),
            pltpu.SemaphoreType.DMA((6,)),
            pltpu.SemaphoreType.DMA((6,)),
            pltpu.SemaphoreType.DMA((3 * GROUPS,)),
            pltpu.SemaphoreType.DMA((3 * GROUPS,)),
        ],
        compiler_params=pltpu.CompilerParams(
            collective_id=0, has_side_effects=True, vmem_limit_bytes=60 * 1024 * 1024
        ),
        name="fused_layer",
    )(
        tokens,
        first_norm_scale.reshape(1, width),
        recurrent_branch_matrix,
        gelu_gate_matrix,
        filter_taps_weight,
        recurrence_gate_blocks,
        input_gate_blocks,
        base_decay_logits.reshape(1, channels),
        extra_log_decay,
        mixer_output_matrix,
        second_norm_scale.reshape(1, width),
        mixer_up_matrix,
        mixer_down_matrix,
    )


def solution(mesh):
    in_specs = (
        P("fs", None),
        P(),
        P("fs", "tp"),
        P("fs", "tp"),
        P(None, "tp"),
        P("tp", None, None),
        P("tp", None, None),
        P("tp"),
        P("fs", "tp"),
        P("fs", "tp"),
        P(),
        P("fs", "tp"),
        P("fs", "tp"),
    )
    out_specs = P(("fs", "tp"), None)
    body = functools.partial(fused_local, mesh) if fits(mesh) else local
    return jax.shard_map(body, mesh=mesh, in_specs=in_specs, out_specs=out_specs, check_vma=False)
```

```python
import functools

import jax
import jax.numpy as jnp
from jax import lax
from jax.experimental import pallas as pl
from jax.experimental.pallas import tpu as pltpu
from jax.sharding import PartitionSpec as P

epsilon = 1e-06
decay_rate_scale = 8.0


def rms_scaled(sequence_token_rows, scales):
    widened = sequence_token_rows.astype(jnp.float32)
    mean_square = jnp.mean(widened * widened, axis=-1, keepdims=True)
    return (widened * lax.rsqrt(mean_square + epsilon) * scales).astype(jnp.bfloat16)


def linear_combine(earlier, later):
    return (earlier[0] * later[0], later[0] * earlier[1] + later[1])


def causal_taps(branch, filter_taps_weight):
    tap_count = filter_taps_weight.shape[0]
    positions = branch.shape[0]
    padded = jnp.pad(branch.astype(jnp.float32), ((tap_count - 1, 0), (0, 0)))
    running = jnp.zeros(branch.shape, jnp.float32)
    for offset in range(tap_count):
        running = running + padded[offset : offset + positions] * filter_taps_weight[offset].astype(
            jnp.float32
        )
    return running.astype(jnp.bfloat16)


def block_map(convolved, blocks):
    positions, channels = convolved.shape
    grouped = convolved.reshape(positions, blocks.shape[0], blocks.shape[1])
    mapped = jnp.einsum("sgi,gij->sgj", grouped, blocks, preferred_element_type=jnp.float32)
    return jax.nn.sigmoid(mapped.reshape(positions, channels))


def contract_columns(left, right):
    return lax.dot_general(
        left, right, (((1,), (1,)), ((), ())), preferred_element_type=jnp.float32
    )


def local(
    tokens,
    first_norm_scale,
    recurrent_branch_matrix,
    gelu_gate_matrix,
    filter_taps_weight,
    recurrence_gate_blocks,
    input_gate_blocks,
    base_decay_logits,
    extra_log_decay,
    mixer_output_matrix,
    second_norm_scale,
    mixer_up_matrix,
    mixer_down_matrix,
):
    positions = tokens.shape[0]
    own_count = positions // lax.axis_size("tp")
    normed = rms_scaled(tokens, first_norm_scale)
    branch_sum = jnp.dot(
        normed,
        lax.all_gather(recurrent_branch_matrix, "fs", axis=0, tiled=True),
        preferred_element_type=jnp.float32,
    )
    gate_sum = jnp.dot(
        normed,
        lax.all_gather(gelu_gate_matrix, "fs", axis=0, tiled=True),
        preferred_element_type=jnp.float32,
    )
    branch = branch_sum.astype(jnp.bfloat16)
    gate_branch = gate_sum.astype(jnp.bfloat16)
    out_full = lax.all_gather(mixer_output_matrix, "fs", axis=0, tiled=True)
    convolved = causal_taps(branch, filter_taps_weight)
    recurrence_gate_value = block_map(convolved, recurrence_gate_blocks)
    admission = block_map(convolved, input_gate_blocks)
    log_keep_factor = (
        decay_rate_scale * recurrence_gate_value * jax.nn.log_sigmoid(base_decay_logits)
        + extra_log_decay
    )
    retain = jnp.exp(log_keep_factor)
    driven = jnp.sqrt(-jnp.expm1(2.0 * log_keep_factor)) * (
        admission * convolved.astype(jnp.float32)
    )
    memory = lax.associative_scan(linear_combine, (retain, driven), axis=0)[1]
    recurrent = (memory * jax.nn.gelu(gate_branch.astype(jnp.float32))).astype(jnp.bfloat16)
    up_full = lax.all_gather(mixer_up_matrix, "fs", axis=0, tiled=True)
    whole_sum = lax.psum(contract_columns(recurrent, out_full).astype(jnp.bfloat16), "tp").astype(
        jnp.float32
    )
    residual_all = (tokens.astype(jnp.float32) + whole_sum).astype(jnp.bfloat16)
    raised = jnp.dot(
        rms_scaled(residual_all, second_norm_scale), up_full, preferred_element_type=jnp.float32
    )
    hidden = jnp.square(jax.nn.relu(raised)).astype(jnp.bfloat16)
    residual = lax.dynamic_slice_in_dim(
        residual_all, lax.axis_index("tp") * own_count, own_count, 0
    )
    down_full = lax.all_gather(mixer_down_matrix, "fs", axis=0, tiled=True)
    channel_sum = lax.psum_scatter(
        contract_columns(hidden, down_full).astype(jnp.bfloat16),
        "tp",
        scatter_dimension=0,
        tiled=True,
    ).astype(jnp.float32)
    return (residual.astype(jnp.float32) + channel_sum).astype(jnp.bfloat16)


MESH = pl.DeviceIdType.MESH
Y_SIZE = 2
GROUPS = 4


def fits(mesh):
    n_fs, n_tp = mesh.shape["fs"], mesh.shape["tp"]
    return n_tp == 2 * Y_SIZE and n_fs == 4 * Y_SIZE


def shifted_down(values, by, fill):
    if by % 8 == 0:
        top = jnp.full((by, values.shape[1]), fill, values.dtype)
        return jnp.concatenate([top, values[: values.shape[0] - by]], axis=0)
    rows = lax.broadcasted_iota(jnp.int32, values.shape, 0)
    return jnp.where(rows < by, fill, pltpu.roll(values, by, 0))


def one_minus_exp(exponent):
    series = 1.0
    for order in range(8, 1, -1):
        series = 1.0 + exponent * (1.0 / order) * series
    return jnp.where(exponent > -0.35, -exponent * series, 1.0 - jnp.exp(exponent))


def fused(
    nz,
    tok_in, scale1, wb, wg, taps, rblk, iblk, logits, extra_in, wo, scale2, wu, wd,
    out,
    normed, fb, fg, fo, fu, fd, rdiag, idiag,
    part, pair1, give2, got2, res, mid, hidden,
    part_f, pair_f, give_f, got_f,
    send_sem, recv_sem, a_send, a_recv, b_send, b_recv, l_sem, tok, extra,
):
    f = lax.axis_index("fs")
    t = lax.axis_index("tp")
    z, y = f // Y_SIZE, f % Y_SIZE
    x, c = t // 2, t % 2
    last = nz - 1
    ymate = z * Y_SIZE + (1 - y)
    xmate = (1 - x) * 2 + c
    cmate = x * 2 + (1 - c)
    rows, width = tok.shape
    own_rows = out.shape[0]
    depth = wb.shape[0]
    half = depth // 2

    early = [
        pltpu.make_async_copy(tok_in, tok, l_sem.at[5]),
        pltpu.make_async_copy(extra_in, extra, l_sem.at[6]),
    ]
    for copy in early:
        copy.start()
    barrier = pltpu.get_barrier_semaphore()
    zup = lax.rem(z + 1, nz) * Y_SIZE + y
    zdown = lax.rem(z + nz - 1, nz) * Y_SIZE + y
    for other in (zup, zdown, ymate):
        pl.semaphore_signal(barrier, inc=1, device_id={"fs": other, "tp": t}, device_id_type=MESH)
    for other in (xmate, cmate):
        pl.semaphore_signal(barrier, inc=1, device_id={"fs": f, "tp": other}, device_id_type=MESH)
    pl.semaphore_wait(barrier, 5)

    pieces = (
        (wb, fb, 0, depth, False),
        (wg, fg, 0, depth, False),
        (wo, fo, 0, depth, True),
        (wu, fu, 0, half, False),
        (wu, fu, half, half, True),
        (wd, fd, 0, half, False),
        (wd, fd, half, half, True),
    )
    sent = []

    def slot(g, shard):
        _, full, first, count, _ = pieces[g]
        return full.at[pl.ds(pl.multiple_of(shard * depth + first, half), count), :]

    def give(g, shard, way, pred, source=None):
        target = (zup, zdown, ymate)[way]
        here = slot(g, shard)
        copy = pltpu.make_async_remote_copy(
            src_ref=here if source is None else source,
            dst_ref=here,
            send_sem=send_sem.at[g, shard, way],
            recv_sem=recv_sem.at[g, shard],
            device_id={"fs": target, "tp": t},
            device_id_type=MESH,
        )
        if pred is None:
            copy.start()
            sent.append((None, copy))
        else:
            pl.when(pred)(copy.start)
            sent.append((pred, copy))

    def take(g, shard):
        here = slot(g, shard)
        pltpu.make_async_remote_copy(
            src_ref=here,
            dst_ref=here,
            send_sem=send_sem.at[g, shard, 0],
            recv_sem=recv_sem.at[g, shard],
            device_id={"fs": ymate, "tp": t},
            device_id_type=MESH,
        ).wait_recv()

    def own(g):
        w, _, first, count, _ = pieces[g]
        source = w.at[pl.ds(first, count), :]
        give(g, f, 0, z < last, source)
        give(g, f, 1, z > 0, source)
        give(g, f, 2, None, source)

    def wave(g, d):
        along = pieces[g][4]
        for way in (0, 1):
            edge = 0 if way == 0 else last
            zs = z - d if way == 0 else z + d
            exists = zs >= 0 if way == 0 else zs <= last
            onward = z < last if way == 0 else z > 0
            if d > 0:
                shard = zs * Y_SIZE + y
                pl.when(exists)(functools.partial(take, g, shard))
                give(g, shard, way, exists & onward)
                if along:
                    give(g, shard, 2, exists & (zs != 0) & (zs != last))
                else:
                    give(g, shard, 2, exists)
            if along:
                outer = zs == edge
                shard = edge * Y_SIZE + (1 - y)
                pl.when(outer)(functools.partial(take, g, shard))
                give(g, shard, way, outer & onward)

    def take_across(g):
        for zs in range(nz):
            if not (pieces[g][4] and zs in (0, last)):
                take(g, zs * Y_SIZE + (1 - y))

    def tp_copy(source, target, other, index, send, recv):
        return pltpu.make_async_remote_copy(
            src_ref=source,
            dst_ref=target,
            send_sem=send.at[index],
            recv_sem=recv.at[index],
            device_id={"fs": f, "tp": other},
            device_id_type=MESH,
        )

    own(0)
    own(1)
    own(2)

    place = pl.ds(pl.multiple_of(f * depth, depth), depth)
    stays = [
        pltpu.make_async_copy(w, full.at[place, :], l_sem.at[i])
        for i, (w, full) in enumerate(((wb, fb), (wg, fg), (wo, fo), (wu, fu), (wd, fd)))
    ]
    for copy in stays:
        copy.start()
    block = rblk.shape[1]
    for blocks, diag in ((rblk, rdiag), (iblk, idiag)):
        diag[...] = jnp.zeros_like(diag)
        for b in range(rblk.shape[0]):
            diag[b * block : (b + 1) * block, b * block : (b + 1) * block] = blocks[b]

    for copy in early:
        copy.wait()

    def norm_rows(i, carry):
        at = pl.ds(pl.multiple_of(i * 32, 32), 32)
        normed[at, :] = rms_scaled(tok[at, :], scale1[...])
        return carry

    lax.fori_loop(0, rows // 32, norm_rows, 0)

    wave(0, 1)
    wave(1, 1)
    own(3)
    wave(2, 0)
    wave(2, 1)
    wave(0, 2)
    wave(1, 2)
    own(4)
    wave(3, 1)
    wave(0, 3)
    wave(1, 3)
    wave(2, 2)
    own(5)
    take_across(0)
    take_across(1)
    for copy in stays:
        copy.wait()

    branch = jnp.dot(normed[...], fb[...], preferred_element_type=jnp.float32)
    branch = branch.astype(jnp.bfloat16).astype(jnp.float32)
    tap_count = taps.shape[0]
    running = branch * taps[tap_count - 1 : tap_count, :].astype(jnp.float32)
    for offset in range(tap_count - 1):
        by = tap_count - 1 - offset
        running = running + shifted_down(branch, by, 0.0) * taps[offset : offset + 1, :].astype(
            jnp.float32
        )
    convolved = running.astype(jnp.bfloat16)
    rate = jax.nn.sigmoid(jnp.dot(convolved, rdiag[...], preferred_element_type=jnp.float32))
    admission = jax.nn.sigmoid(jnp.dot(convolved, idiag[...], preferred_element_type=jnp.float32))
    base = -jnp.log1p(jnp.exp(-logits[...]))
    log_keep = decay_rate_scale * rate * base + extra[...]
    keep = jnp.exp(log_keep)
    memory = jnp.sqrt(one_minus_exp(2.0 * log_keep)) * (admission * convolved.astype(jnp.float32))
    by = 1
    while by < rows:
        memory = keep * shifted_down(memory, by, 0.0) + memory
        if 2 * by < rows:
            keep = keep * shifted_down(keep, by, 1.0)
        by *= 2
    gate = jnp.dot(normed[...], fg[...], preferred_element_type=jnp.float32)
    gate = gate.astype(jnp.bfloat16).astype(jnp.float32)
    recurrent = (memory * jax.nn.gelu(gate)).astype(jnp.bfloat16)

    wave(2, 3)
    wave(3, 2)
    own(6)
    take_across(2)
    for k in range(width // depth):
        product = contract_columns(recurrent, fo[k * depth : (k + 1) * depth, :])
        part[:, :, k * depth : (k + 1) * depth] = product.astype(jnp.bfloat16).reshape(
            part.shape[0], own_rows, depth
        )
    first = [
        tp_copy(part.at[2 * other + (1 - c)], pair1.at[other], cmate, other, a_send, a_recv)
        for other in range(2)
    ]
    for copy in first:
        copy.start()
    wave(4, 0)
    for copy in first:
        copy.wait_recv()
    away = part[2 * (1 - x) + c].astype(jnp.float32) + pair1[1 - x].astype(jnp.float32)
    give2[...] = away.astype(jnp.bfloat16)
    second = tp_copy(give2, got2, xmate, 2, a_send, a_recv)
    second.start()
    wave(4, 1)
    wave(3, 3)
    second.wait_recv()
    own_at = pl.ds(pl.multiple_of(t * own_rows, own_rows), own_rows)
    mixed = part[t].astype(jnp.float32) + pair1[x].astype(jnp.float32)
    mixed = mixed + got2[...].astype(jnp.float32)
    residual = (tok[own_at, :].astype(jnp.float32) + mixed).astype(jnp.bfloat16)
    res[...] = residual
    mid[t] = rms_scaled(residual, scale2[...])
    spread = [
        tp_copy(mid.at[t], mid.at[t], xmate, 3, a_send, a_recv),
        tp_copy(mid.at[t], mid.at[t], cmate, 4, a_send, a_recv),
    ]
    for copy in spread:
        copy.start()
    wave(4, 2)
    wave(5, 1)
    tp_copy(mid.at[xmate], mid.at[xmate], xmate, 3, a_send, a_recv).wait_recv()
    relay = tp_copy(mid.at[xmate], mid.at[xmate], cmate, 5, a_send, a_recv)
    relay.start()
    wave(4, 3)
    wave(5, 2)
    tp_copy(mid.at[cmate], mid.at[cmate], cmate, 4, a_send, a_recv).wait_recv()
    diagonal = (1 - x) * 2 + (1 - c)
    tp_copy(mid.at[diagonal], mid.at[diagonal], cmate, 5, a_send, a_recv).wait_recv()
    wave(6, 0)
    wave(6, 1)
    take_across(3)
    take_across(4)

    tile = 256

    def up_tile(i, carry):
        at = pl.ds(pl.multiple_of(i * tile, tile), tile)
        raised = jnp.dot(
            mid[...].reshape(rows, width), fu[:, at], preferred_element_type=jnp.float32
        )
        hidden[:, at] = jnp.square(jnp.maximum(raised, 0.0)).astype(jnp.bfloat16)
        return carry

    lax.fori_loop(0, fu.shape[1] // tile, up_tile, 0)

    span = width // GROUPS
    side = z // (nz // 2)
    inner = z + side * (last - 2 * z)
    ranks = [inner, 1 - inner] + list(range(2, nz))
    order = [rank + side * (last - 2 * rank) for rank in ranks]
    firsts, seconds = [], []

    def finish_first(j):
        for copy in firsts[j]:
            copy.wait_recv()
        away = part_f[j, 2 * (1 - x) + c].astype(jnp.float32) + pair_f[j, 1 - x].astype(jnp.float32)
        give_f[j] = away.astype(jnp.bfloat16)
        copy = tp_copy(give_f.at[j], got_f.at[j], xmate, 3 * j + 2, b_send, b_recv)
        copy.start()
        seconds.append(copy)

    def columns(j):
        return pl.ds(pl.multiple_of(order[j] * span, span), span)

    def finish_second(j):
        seconds[j].wait_recv()
        total = part_f[j, t].astype(jnp.float32) + pair_f[j, x].astype(jnp.float32)
        total = total + got_f[j].astype(jnp.float32)
        out[:, columns(j)] = (res[:, columns(j)].astype(jnp.float32) + total).astype(jnp.bfloat16)

    for j in range(GROUPS):
        if j == 1:
            wave(5, 3)
        if j > 1:
            wave(6, j)
        q = order[j]
        take(5, q * Y_SIZE + (1 - y))
        if j != last:
            pl.when((q != 0) & (q != last))(functools.partial(take, 6, q * Y_SIZE + (1 - y)))
        product = contract_columns(hidden[...], fd[columns(j), :])
        part_f[j] = product.astype(jnp.bfloat16).reshape(part.shape[0], own_rows, span)
        copies = [
            tp_copy(
                part_f.at[j, 2 * other + (1 - c)], pair_f.at[j, other], cmate, 3 * j + other,
                b_send, b_recv,
            )
            for other in range(2)
        ]
        for copy in copies:
            copy.start()
        firsts.append(copies)
        if j > 0:
            finish_first(j - 1)
        if j > 1:
            finish_second(j - 2)
    finish_first(GROUPS - 1)
    finish_second(GROUPS - 2)
    finish_second(GROUPS - 1)

    for pred, copy in sent:
        if pred is None:
            copy.wait_send()
        else:
            pl.when(pred)(copy.wait_send)
    for copy in first + [second] + spread + [relay] + seconds:
        copy.wait_send()
    for copies in firsts:
        for copy in copies:
            copy.wait_send()


def fused_local(
    mesh,
    tokens,
    first_norm_scale,
    recurrent_branch_matrix,
    gelu_gate_matrix,
    filter_taps_weight,
    recurrence_gate_blocks,
    input_gate_blocks,
    base_decay_logits,
    extra_log_decay,
    mixer_output_matrix,
    second_norm_scale,
    mixer_up_matrix,
    mixer_down_matrix,
):
    n_fs, n_tp = mesh.shape["fs"], mesh.shape["tp"]
    rows, width = tokens.shape
    own_rows = rows // n_tp
    channels = recurrent_branch_matrix.shape[1]
    units = mixer_up_matrix.shape[1]
    span = width // GROUPS
    low, high = jnp.bfloat16, jnp.float32
    vmem = pl.BlockSpec(memory_space=pltpu.VMEM)
    hbm = pl.BlockSpec(memory_space=pl.ANY)
    return pl.pallas_call(
        functools.partial(fused, n_fs // Y_SIZE),
        out_shape=jax.ShapeDtypeStruct((own_rows, width), low),
        in_specs=[hbm, vmem, hbm, hbm] + [vmem] * 4 + [hbm, hbm, vmem, hbm, hbm],
        out_specs=vmem,
        scratch_shapes=[
            pltpu.VMEM((rows, width), low),
            pltpu.VMEM((width, channels), low),
            pltpu.VMEM((width, channels), low),
            pltpu.VMEM((width, channels), low),
            pltpu.VMEM((width, units), low),
            pltpu.VMEM((width, units), low),
            pltpu.VMEM((channels, channels), low),
            pltpu.VMEM((channels, channels), low),
            pltpu.VMEM((n_tp, own_rows, width), low),
            pltpu.VMEM((2, own_rows, width), low),
            pltpu.VMEM((own_rows, width), low),
            pltpu.VMEM((own_rows, width), low),
            pltpu.VMEM((own_rows, width), low),
            pltpu.VMEM((n_tp, own_rows, width), low),
            pltpu.VMEM((rows, units), low),
            pltpu.VMEM((GROUPS, n_tp, own_rows, span), low),
            pltpu.VMEM((GROUPS, 2, own_rows, span), low),
            pltpu.VMEM((GROUPS, own_rows, span), low),
            pltpu.VMEM((GROUPS, own_rows, span), low),
            pltpu.SemaphoreType.DMA((7, n_fs, 3)),
            pltpu.SemaphoreType.DMA((7, n_fs)),
            pltpu.SemaphoreType.DMA((6,)),
            pltpu.SemaphoreType.DMA((6,)),
            pltpu.SemaphoreType.DMA((3 * GROUPS,)),
            pltpu.SemaphoreType.DMA((3 * GROUPS,)),
            pltpu.SemaphoreType.DMA((7,)),
            pltpu.VMEM((rows, width), low),
            pltpu.VMEM((rows, channels), high),
        ],
        compiler_params=pltpu.CompilerParams(
            collective_id=0, has_side_effects=True, vmem_limit_bytes=60 * 1024 * 1024
        ),
        name="fused_layer",
    )(
        tokens,
        first_norm_scale.reshape(1, width),
        recurrent_branch_matrix,
        gelu_gate_matrix,
        filter_taps_weight,
        recurrence_gate_blocks,
        input_gate_blocks,
        base_decay_logits.reshape(1, channels),
        extra_log_decay,
        mixer_output_matrix,
        second_norm_scale.reshape(1, width),
        mixer_up_matrix,
        mixer_down_matrix,
    )


def solution(mesh):
    in_specs = (
        P("fs", None),
        P(),
        P("fs", "tp"),
        P("fs", "tp"),
        P(None, "tp"),
        P("tp", None, None),
        P("tp", None, None),
        P("tp"),
        P("fs", "tp"),
        P("fs", "tp"),
        P(),
        P("fs", "tp"),
        P("fs", "tp"),
    )
    out_specs = P(("fs", "tp"), None)
    body = functools.partial(fused_local, mesh) if fits(mesh) else local
    return jax.shard_map(body, mesh=mesh, in_specs=in_specs, out_specs=out_specs, check_vma=False)
```
